32 devices in a mesh: sp: 8 (over z, x), dp: 4 (over y, core).
Axes of the slice: x: 2, y: 2, z: 4, core: 2. Of those that a mesh axis runs over, the one named last changes fastest.
Arguments:
- layer_activity: bfloat16 [4, 1024, 2048], P('dp', 'sp'), may hold values from -6 to 6
- writer_matrix: bfloat16 [2048, 256], P('dp'), may hold values from -0.125 to 0.125
- reader_matrix: bfloat16 [2048, 256], P('dp'), may hold values from -0.125 to 0.125
- source_unfiltered: bfloat16 [4, 1024, 2048], P('dp', 'sp'), may hold values from -6 to 6
- switch_raw_signal: bfloat16 [4, 1024, 2048], P('dp', 'sp'), may hold values from -6 to 6
- saved_result: bfloat16 [4, 1024, 2048], P('dp', 'sp'), may hold values from -6 to 6
- final_adjoint: bfloat16 [4, 1024, 2048], P('dp', 'sp'), may hold values from -6 to 6
- delta_raw: bfloat16 [4, 1024, 32], P('dp', 'sp'), may hold values from -4 to 4
- extra_logdrop: float32 [4, 1024, 32], P('dp', None, 'sp'), may hold values from 0 to 2.1
- source_filter_coefs: float32 [5, 2048], P(None, 'sp'), may hold values from -2.5 to 2.5
- writer_filter_coefs: float32 [5, 256], replicated, may hold values from -2.5 to 2.5
- reader_filter_coefs: float32 [5, 256], replicated, may hold values from -2.5 to 2.5
- delta_offset: float32 [32], P('sp'), may hold values from -7.5 to -6
- fading_exponents: float32 [32], P('sp'), may hold values from -6 to 3.4
- direct_factor: float32 [32], P('sp'), may hold values from 0.1 to 1.9
- rescale_factor: float32 [2048], replicated, may hold values from 0.1 to 1.9
Outputs:
- d_hidden: bfloat16 [4, 1024, 2048], P('dp', 'sp')
- d_x_raw: bfloat16 [4, 1024, 2048], P('dp', 'sp')
- d_gate: bfloat16 [4, 1024, 2048], P('dp', 'sp')
- d_dt_raw: bfloat16 [4, 1024, 32], P('dp', 'sp')
- d_w_b: float32 [2048, 256], P('dp')
- d_w_c: float32 [2048, 256], P('dp')
The draws below stay inside these ranges and needn't reach their ends.
All inputs are finite; a program needn't handle non-finite values.
Results may differ from the reference program's by a relative error of at most 0.012.
Values may be sent and summed in bfloat16 or wider, within the bound.
A program may use at most 128 MiB of HBM per device.

```python
import jax
import jax.numpy as jnp
from jax import lax

D = 2048
HEADS = 32
HEAD_DIM = 64
STATE = 128
GROUPS = 2
NORM_GROUPS = 8
CONV_K = 5
BLOCK = 128
TOK_DEV = 128
INNER = 2048
TOKEN_TOTAL = 1024
BATCH_TOTAL = 4


def draw_delta_raw(key, part):
    key_base, key_shift = jax.random.split(key)
    baseline = jnp.clip(0.7 * jax.random.normal(key_base, (BATCH_TOTAL, TOKEN_TOTAL, HEADS), jnp.float32), -2.8, 2.8)
    blocks = TOKEN_TOTAL // TOK_DEV
    shifts = jax.random.uniform(key_shift, (BATCH_TOTAL, blocks, 1, 1), jnp.float32, -1.0, 1.0)
    shifts = jnp.broadcast_to(shifts, (BATCH_TOTAL, blocks, TOK_DEV, 1)).reshape(BATCH_TOTAL, TOKEN_TOTAL, 1)
    return (baseline + shifts).astype(jnp.bfloat16)


def draw_extra_logdrop(key, part):
    key_where, key_size = jax.random.split(key)
    places = jax.random.randint(key_where, (3, BATCH_TOTAL, 1, HEADS), 0, TOKEN_TOTAL)
    amounts = jax.random.uniform(key_size, (3, BATCH_TOTAL, 1, HEADS), jnp.float32, 0.22, 0.69)
    positions = jnp.arange(TOKEN_TOTAL, dtype=jnp.int32)[None, None, :, None]
    return jnp.sum(jnp.where(positions == places, amounts, 0.0), axis=0)


def draw_fading_exponents(key, part):
    key_pick, key_fast, key_slow = jax.random.split(key, 3)
    fraction = 0.5
    picked = jax.random.uniform(key_pick, (HEADS,), jnp.float32) < fraction
    fast_rate = jax.random.uniform(key_fast, (HEADS,), jnp.float32, 2.3, 3.0)
    slow_rate = jnp.log(jax.random.uniform(key_slow, (HEADS,), jnp.float32, 0.2, 0.8) / (TOKEN_TOTAL * 0.0018))
    return jnp.where(picked, fast_rate, slow_rate)


def strengthened(result, key, source, target, blocks, factor):
    owner, partner = [(jnp.arange(result.shape[position]) // (result.shape[position] // blocks)).reshape([-1 if axis == position else 1 for axis in range(result.ndim)]) for position in (source, target)]
    chosen = jax.random.permutation(key, blocks)[partner]
    strong = (owner == chosen) | (owner == (partner + blocks // 2) % blocks)
    return jnp.where(strong, factor * result, result)


def level_of(stream_key, extent, cuts, smallest, high):
    factor_of = 1.0
    for axis_at, shards_of in cuts:
        heights = jax.random.uniform(jax.random.fold_in(jax.random.fold_in(stream_key, 6), axis_at), (shards_of,), jnp.float32, smallest / len(cuts), high / len(cuts))
        factor_of = factor_of * jnp.repeat(jnp.exp(heights), extent[axis_at] // shards_of).reshape((-1,) + (1,) * (len(extent) - 1 - axis_at))
    return factor_of


def gaussian(key, extent, spread, most, pieces=(), held_as=jnp.bfloat16):
    values = jax.random.normal(key, extent, jnp.float32) * spread
    if len(pieces) > 0:
        values = level_of(key, extent, pieces, -0.22, 0.18) * values
    return jnp.clip(values, min=-most, max=most).astype(held_as)


def bell_draw_with(rng, dims, scale, bound, shards, heavy, kind=jnp.bfloat16):
    entries = scale * jax.random.normal(rng, dims, jnp.float32)
    if shards:
        entries = entries * level_of(rng, dims, shards, -0.22, 0.18)
    return jnp.clip(strengthened(entries, jax.random.fold_in(rng, 3), *heavy), -bound, bound).astype(kind)


def setup_inputs(seed: int = 0) -> dict:
    seeds = jax.random.split(jax.random.key(seed), 17)
    return {
        "layer_activity": bell_draw_with(seeds[0], (BATCH_TOTAL, TOKEN_TOTAL, D), 1.0, 6.0, ((0, 4), (1, 8)), (1, 2, 8, 2.0)),
        "writer_matrix": gaussian(seeds[1], (D, GROUPS * STATE), D ** -0.5, 0.125, ((0, 4),)),
        "reader_matrix": gaussian(seeds[2], (D, GROUPS * STATE), D ** -0.5, 0.125, ((0, 4),)),
        "source_unfiltered": gaussian(seeds[3], (BATCH_TOTAL, TOKEN_TOTAL, INNER), 1.0, 6.0, ((0, 4), (1, 8))),
        "switch_raw_signal": gaussian(seeds[4], (BATCH_TOTAL, TOKEN_TOTAL, INNER), 1.0, 6.0, ((0, 4), (1, 8))),
        "saved_result": gaussian(seeds[5], (BATCH_TOTAL, TOKEN_TOTAL, INNER), 1.0, 6.0, ((0, 4), (1, 8))),
        "final_adjoint": gaussian(seeds[6], (BATCH_TOTAL, TOKEN_TOTAL, INNER), 1.0, 6.0, ((0, 4), (1, 8))),
        "delta_raw": draw_delta_raw(jax.random.fold_in(seeds[16], 71), 0),
        "extra_logdrop": draw_extra_logdrop(jax.random.fold_in(seeds[16], 71), 0),
        "source_filter_coefs": gaussian(seeds[9], (CONV_K, INNER), CONV_K ** -0.5, 2.5, ((1, 8),), jnp.float32),
        "writer_filter_coefs": gaussian(seeds[10], (CONV_K, GROUPS * STATE), CONV_K ** -0.5, 2.5, (), jnp.float32),
        "reader_filter_coefs": gaussian(seeds[11], (CONV_K, GROUPS * STATE), CONV_K ** -0.5, 2.5, (), jnp.float32),
        "delta_offset": jnp.clip(-7.5 + 1.5 * jax.random.uniform(seeds[12], (HEADS,), jnp.float32) ** level_of(seeds[12], (HEADS,), ((0, 8),), -0.2, 0.2), -7.5, -6.0),
        "fading_exponents": draw_fading_exponents(jax.random.fold_in(seeds[16], 71), 0),
        "direct_factor": jnp.clip(1.0 + 0.18 * jax.random.normal(seeds[14], (HEADS,), jnp.float32), 0.1, 1.9),
        "rescale_factor": jnp.clip(1.0 + 0.18 * jax.random.normal(seeds[15], (INNER,), jnp.float32), 0.1, 1.9),
    }


EPSILON = 1e-06
highest = lax.Precision.HIGHEST

def centred_conv(values, tap_weights):
    sample_window = values.shape[0]
    reach_side = (tap_weights.shape[0] - 1) // 2
    padded = jnp.pad(values, ((reach_side, reach_side), (0, 0)))
    summed = jnp.zeros_like(values)
    for offset in range(tap_weights.shape[0]):
        summed = summed + tap_weights[offset][None, :] * padded[offset:offset + sample_window]
    return summed

def one_channel_scan(source_unfiltered, writer_unfiltered, reader_unfiltered, delta_raw, extra_logdrop, source_filter_coefs, writer_filter_coefs, reader_filter_coefs, delta_offset, fading_exponents, direct_factor):
    inputs = jax.nn.silu(centred_conv(source_unfiltered, source_filter_coefs))
    keys_b = jax.nn.silu(centred_conv(writer_unfiltered, writer_filter_coefs))
    reads_c = jax.nn.silu(centred_conv(reader_unfiltered, reader_filter_coefs))
    smooth_delta = jax.nn.softplus(delta_raw + delta_offset)
    channel_fading = smooth_delta * jnp.exp(fading_exponents) + extra_logdrop
    cumulative = jnp.cumsum(channel_fading)
    sample_window = source_unfiltered.shape[0]
    blocks = sample_window // BLOCK
    driven = (inputs * smooth_delta[:, None]).reshape(blocks, BLOCK, -1)
    keyed = keys_b.reshape(blocks, BLOCK, -1)
    reading = reads_c.reshape(blocks, BLOCK, -1)
    levels = cumulative.reshape(blocks, BLOCK)
    within = jnp.exp(-jnp.abs(levels[:, :, None] - levels[:, None, :]))
    scores = jnp.einsum('ktn,ksn->kts', reading, keyed, precision=highest) * within
    output = jnp.einsum('kts,ksp->ktp', scores, driven, precision=highest)
    block_ends = levels[:, -1]
    block_starts = levels[:, 0]
    block_order = jnp.arange(blocks, dtype=jnp.int32)
    prev_end = jnp.concatenate([cumulative[:1], block_ends[:-1]])
    next_start = jnp.concatenate([block_starts[1:], cumulative[-1:]])
    weight_fwd = jnp.exp(levels - block_ends[:, None])
    state_fwd = jnp.einsum('ksn,ksp->knp', keyed * weight_fwd[:, :, None], driven, precision=highest)
    mask_fwd = (block_order[None, :] < block_order[:, None]).astype(cumulative.dtype)
    link_fwd = jnp.exp(-jnp.abs(prev_end[:, None] - block_ends[None, :])) * mask_fwd
    carry_fwd = jnp.einsum('kj,jnp->knp', link_fwd, state_fwd, precision=highest)
    read_fwd = reading * jnp.exp(prev_end[:, None] - levels)[:, :, None]
    weight_bwd = jnp.exp(block_starts[:, None] - levels)
    state_bwd = jnp.einsum('ksn,ksp->knp', keyed * weight_bwd[:, :, None], driven, precision=highest)
    mask_bwd = (block_order[None, :] > block_order[:, None]).astype(cumulative.dtype)
    link_bwd = jnp.exp(-jnp.abs(next_start[:, None] - block_starts[None, :])) * mask_bwd
    carry_bwd = jnp.einsum('kj,jnp->knp', link_bwd, state_bwd, precision=highest)
    read_bwd = reading * jnp.exp(levels - next_start[:, None])[:, :, None]
    output = output + jnp.einsum('ktn,knp->ktp', read_fwd, carry_fwd, precision=highest)
    output = output + jnp.einsum('ktn,knp->ktp', read_bwd, carry_bwd, precision=highest)
    return output.reshape(sample_window, -1) + direct_factor * inputs

def channelwise_derivs(source_unfiltered, writer_unfiltered, reader_unfiltered, delta_raw, extra_logdrop, source_filter_coefs, writer_filter_coefs, reader_filter_coefs, delta_offset, fading_exponents, direct_factor, result_adjoint):

    def forward(source_filtered, writer_filtered, reader_filtered, delta_argument):
        return one_channel_scan(source_filtered, writer_filtered, reader_filtered, delta_argument, extra_logdrop, source_filter_coefs, writer_filter_coefs, reader_filter_coefs, delta_offset, fading_exponents, direct_factor)
    primal, pullback = jax.vjp(forward, source_unfiltered.astype(jnp.float32), writer_unfiltered.astype(jnp.float32), reader_unfiltered.astype(jnp.float32), delta_raw.astype(jnp.float32))
    source_derivative, writer_derivative, reader_derivative, delta_derivative = pullback(result_adjoint.astype(jnp.float32))
    return (source_derivative.astype(jnp.bfloat16), writer_derivative.astype(jnp.bfloat16), reader_derivative.astype(jnp.bfloat16), delta_derivative.astype(jnp.bfloat16))

def gated_norm(values, gating, rescale_factor):
    mixed = values * jax.nn.silu(gating)
    grouped = mixed.reshape(mixed.shape[0], NORM_GROUPS, -1)
    scaled = grouped * lax.rsqrt(lax.optimization_barrier(jnp.mean(grouped * grouped, axis=-1, keepdims=True)) + EPSILON)
    return scaled.reshape(mixed.shape) * rescale_factor

def norm_backward(saved_result, switch_raw_signal, final_adjoint, rescale_factor):
    primal, pullback = jax.vjp(lambda values, gating: gated_norm(values, gating, rescale_factor), saved_result.astype(jnp.float32), switch_raw_signal.astype(jnp.float32))
    d_values, d_gates = pullback(final_adjoint.astype(jnp.float32))
    return (d_values.astype(jnp.bfloat16), d_gates.astype(jnp.bfloat16))

def reference(layer_activity, writer_matrix, reader_matrix, source_unfiltered, switch_raw_signal, saved_result, final_adjoint, delta_raw, extra_logdrop, source_filter_coefs, writer_filter_coefs, reader_filter_coefs, delta_offset, fading_exponents, direct_factor, rescale_factor):
    latent_dimension = GROUPS * STATE
    per_group = HEADS // GROUPS
    group_of = jnp.arange(HEADS, dtype=jnp.int32) // per_group
    token_rows = layer_activity.reshape(BATCH_TOTAL * TOKEN_TOTAL, D)
    writer_linear = jnp.dot(token_rows, writer_matrix, preferred_element_type=jnp.float32).astype(jnp.bfloat16)
    reader_linear = jnp.dot(token_rows, reader_matrix, preferred_element_type=jnp.float32).astype(jnp.bfloat16)
    source_filter_fn = jnp.transpose(source_filter_coefs.reshape(CONV_K, HEADS, HEAD_DIM), (1, 0, 2))
    writer_filter_fn = jnp.transpose(writer_filter_coefs.reshape(CONV_K, GROUPS, STATE)[:, group_of], (1, 0, 2))
    reader_filter_fn = jnp.transpose(reader_filter_coefs.reshape(CONV_K, GROUPS, STATE)[:, group_of], (1, 0, 2))

    def one_sample_pass(collected_parts):
        sample_source, sample_writer, sample_reader, sample_delta, sample_logdrop_lines, sample_result, sample_switch, sample_final = collected_parts
        result_adjoint, d_gate = norm_backward(sample_result, sample_switch, sample_final, rescale_factor)
        channelwise_source = jnp.transpose(sample_source.reshape(TOKEN_TOTAL, HEADS, HEAD_DIM), (1, 0, 2))
        channelwise_writer = jnp.transpose(sample_writer.reshape(TOKEN_TOTAL, GROUPS, STATE)[:, group_of], (1, 0, 2))
        channelwise_reader = jnp.transpose(sample_reader.reshape(TOKEN_TOTAL, GROUPS, STATE)[:, group_of], (1, 0, 2))
        channelwise_adjoint = jnp.transpose(result_adjoint.reshape(TOKEN_TOTAL, HEADS, HEAD_DIM), (1, 0, 2))
        source_derivative, writer_derivative, reader_derivative, delta_derivative = lax.map(lambda collected_items: channelwise_derivs(*collected_items), (channelwise_source, channelwise_writer, channelwise_reader, sample_delta.T, sample_logdrop_lines.T, source_filter_fn, writer_filter_fn, reader_filter_fn, delta_offset, fading_exponents, direct_factor, channelwise_adjoint))
        summed_b = lax.optimization_barrier(jnp.sum(writer_derivative.astype(jnp.float32).reshape(GROUPS, per_group, TOKEN_TOTAL, STATE), axis=1))
        summed_c = lax.optimization_barrier(jnp.sum(reader_derivative.astype(jnp.float32).reshape(GROUPS, per_group, TOKEN_TOTAL, STATE), axis=1))
        summed_b = jnp.transpose(summed_b, (1, 0, 2)).reshape(TOKEN_TOTAL, latent_dimension).astype(jnp.bfloat16)
        summed_c = jnp.transpose(summed_c, (1, 0, 2)).reshape(TOKEN_TOTAL, latent_dimension).astype(jnp.bfloat16)
        return (jnp.transpose(source_derivative, (1, 0, 2)).reshape(TOKEN_TOTAL, INNER), summed_b, summed_c, delta_derivative.T, d_gate)
    whole_batch_source, whole_batch_writer, whole_batch_reader, whole_batch_delta, whole_batch_switch = lax.map(one_sample_pass, (source_unfiltered, writer_linear.reshape(BATCH_TOTAL, TOKEN_TOTAL, latent_dimension), reader_linear.reshape(BATCH_TOTAL, TOKEN_TOTAL, latent_dimension), delta_raw, extra_logdrop, saved_result, switch_raw_signal, final_adjoint))
    grad_rows_b = whole_batch_writer.reshape(BATCH_TOTAL * TOKEN_TOTAL, latent_dimension)
    grad_rows_c = whole_batch_reader.reshape(BATCH_TOTAL * TOKEN_TOTAL, latent_dimension)
    d_hidden = (jnp.dot(grad_rows_b, writer_matrix.T, preferred_element_type=jnp.float32) + jnp.dot(grad_rows_c, reader_matrix.T, preferred_element_type=jnp.float32)).astype(jnp.bfloat16)
    d_w_b = jnp.dot(token_rows.T, grad_rows_b, preferred_element_type=jnp.float32)
    d_w_c = jnp.dot(token_rows.T, grad_rows_c, preferred_element_type=jnp.float32)
    return (d_hidden.reshape(BATCH_TOTAL, TOKEN_TOTAL, D), whole_batch_source, whole_batch_switch, whole_batch_delta, d_w_b, d_w_c)
```

```python
import functools

import jax
import jax.numpy as jnp
from jax import lax
from jax.experimental import pallas as pl
from jax.experimental.pallas import tpu as pltpu
from jax.sharding import PartitionSpec as P

HEADS = 32
HEAD_DIM = 64
STATE = 128
GROUPS = 2
NORM_GROUPS = 8
CONV_K = 5
BLOCK = 128
INNER = 2048
LANES = 128
HALO = 8
EPSILON = 1e-06
LOG2E = 1.4426950408889634
highest = lax.Precision.HIGHEST
f32 = jnp.float32
bf16 = jnp.bfloat16


def sigmoid(v):
    return 1.0 / (1.0 + jnp.exp(-v))


def softplus(v):
    e = jnp.exp(-jnp.abs(v))
    z = e / (2.0 + e)
    z2 = z * z
    series = jnp.full_like(z, 1.0 / 17.0)
    for odd in (15, 13, 11, 9, 7, 5, 3, 1):
        series = series * z2 + 1.0 / odd
    return jnp.maximum(v, 0.0) + 2.0 * z * series


def norm_kernel(values_ref, gates_ref, adjoint_ref, scale_ref, dy_ref, dgate_ref):
    values = values_ref[...].astype(f32)
    gates = gates_ref[...].astype(f32)
    sig = sigmoid(gates)
    act = gates * sig
    g = values * act
    dn = adjoint_ref[...].astype(f32) * scale_ref[...]
    width = g.shape[1]
    inv = lax.rsqrt(jnp.sum(g * g, axis=1, keepdims=True) * (1.0 / width) + EPSILON)
    along = jnp.sum(dn * g, axis=1, keepdims=True) * (1.0 / width)
    dg = inv * dn - g * (inv * inv * inv * along)
    dy_ref[...] = (dg * act).astype(bf16)
    dgate_ref[...] = (dg * values * (sig + act * (1.0 - sig))).astype(bf16)


def norm_backward(values, gates, adjoint, scale):
    tokens, inner = values.shape
    width = inner // NORM_GROUPS
    block = pl.BlockSpec((tokens, width), lambda i: (0, i))
    return pl.pallas_call(
        norm_kernel,
        grid=(NORM_GROUPS,),
        in_specs=[block, block, block, pl.BlockSpec((1, width), lambda i: (0, i))],
        out_specs=[block, block],
        out_shape=[jax.ShapeDtypeStruct((tokens, inner), bf16)] * 2,
        name="norm_backward",
    )(values, gates, adjoint, scale.reshape(1, inner))


def window_conv(padded, r0, taps, flip):
    rows = padded[pl.ds(r0, BLOCK + 2 * HALO), :]
    total = None
    for k in range(CONV_K):
        shift = HALO - CONV_K // 2 + k
        tap = taps[CONV_K - 1 - k if flip else k][None, :]
        term = tap * pltpu.roll(rows, rows.shape[0] - shift, axis=0)[:BLOCK]
        total = term if total is None else total + term
    return total


def mixer_kernel(
    heads,
    tile,
    p1_ref,
    p2_ref,
    drop_ref,
    tapx_ref,
    tapbc_ref,
    par_ref,
    out_ref,
    pad_x,
    pad_bc,
    u_ref,
    sux_ref,
    sbc_ref,
    dtc_ref,
    sig_ref,
    lcol,
    lrow,
    kt,
    rt,
    kn,
    rn,
    vt,
    dyt,
    dyh,
    dvt,
    dkt,
    dr,
    rowacc,
    rowdl,
    colsum,
):
    window = p1_ref.shape[0]
    xw = u_ref.shape[1]
    chunks = window // BLOCK
    tapx = tapx_ref[...]
    tapbc = tapbc_ref[...]
    offset = par_ref[0:1, :]
    fade = par_ref[1:2, :]
    skip = tapx[CONV_K : CONV_K + 1]
    lane_head = lax.broadcasted_iota(jnp.int32, (BLOCK, xw), 1) // HEAD_DIM
    row_i = lax.broadcasted_iota(jnp.int32, (BLOCK, BLOCK), 0)
    col_i = lax.broadcasted_iota(jnp.int32, (BLOCK, BLOCK), 1)
    lower = (row_i >= col_i).astype(f32)
    upper = (row_i <= col_i).astype(f32)

    def spread(columns):
        out = jnp.zeros((BLOCK, xw), f32)
        for h in range(heads):
            out = jnp.where(lane_head == h, columns[:, h : h + 1], out)
        return out

    for padded in (pad_x, pad_bc):
        padded[0:HALO, :] = jnp.zeros((HALO, padded.shape[1]), f32)
        padded[HALO + window :, :] = jnp.zeros((HALO, padded.shape[1]), f32)

    @pl.loop(0, chunks)
    def _(c):
        r0 = pl.multiple_of(c * BLOCK, BLOCK)
        rows = pl.ds(r0, BLOCK)
        into = pl.ds(pl.multiple_of(r0 + HALO, HALO), BLOCK)
        pad_x[into, :] = p1_ref[rows, :xw].astype(f32)
        pad_bc[into, :] = p2_ref[rows, xw:].astype(f32)

    def prepare(c, carry):
        r0 = pl.multiple_of(c * BLOCK, BLOCK)
        rows = pl.ds(r0, BLOCK)
        a = p1_ref[rows, xw:].astype(f32) + offset
        dt = softplus(a)
        dtc_ref[rows, :] = dt
        sig_ref[rows, :] = sigmoid(a)
        rate = dt * fade + drop_ref[rows, :]
        level = jnp.dot(lower, rate, precision=highest, preferred_element_type=f32) + carry
        scaled = level * LOG2E
        lcol[rows, :] = scaled
        lrow[:, rows] = scaled.T[: lrow.shape[0]]
        pre = window_conv(pad_x, r0, tapx, False)
        sig = sigmoid(pre)
        u = pre * sig
        u_ref[rows, :] = u
        sux_ref[rows, :] = sig + u * (1.0 - sig)
        vt[:, rows] = (u * spread(dt)).T.astype(bf16)
        dy_t = p2_ref[rows, :xw].astype(f32).T
        dyt[:, rows] = dy_t.astype(bf16)
        for h in range(heads):
            dyh[h, rows, :] = dy_t[h * HEAD_DIM : (h + 1) * HEAD_DIM].T.astype(bf16)
        pre = window_conv(pad_bc, r0, tapbc, False)
        sig = sigmoid(pre)
        kr = pre * sig
        sbc_ref[rows, :] = sig + kr * (1.0 - sig)
        kn[rows, :] = kr[:, :STATE].astype(bf16)
        rn[rows, :] = kr[:, STATE:].astype(bf16)
        kt[:, rows] = kr[:, :STATE].T.astype(bf16)
        rt[:, rows] = kr[:, STATE:].T.astype(bf16)
        return level[BLOCK - 1 : BLOCK]

    lax.fori_loop(0, chunks, prepare, jnp.zeros((1, LANES), f32))

    dvt[...] = jnp.zeros_like(dvt)
    dkt[...] = jnp.zeros_like(dkt)
    colsum[...] = jnp.zeros_like(colsum)
    rowdl[...] = jnp.zeros_like(rowdl)
    ahead = lax.broadcasted_iota(jnp.int32, (tile, tile), 0) - lax.broadcasted_iota(
        jnp.int32, (tile, tile), 1
    )

    @pl.loop(0, window // tile)
    def _(ti):
        t0 = pl.multiple_of(ti * tile, tile)
        ts = pl.ds(t0, tile)
        rowacc[...] = jnp.zeros_like(rowacc)
        dr[ts, :] = jnp.zeros((tile, STATE), f32)
        reads = rn[ts, :]
        reads_t = rt[:, ts]

        @pl.loop(0, window // tile)
        def _(si):
            s0 = pl.multiple_of(si * tile, tile)
            ss = pl.ds(s0, tile)
            score = jnp.dot(reads, kt[:, ss], preferred_element_type=f32)
            order = jnp.clip(ahead + (t0 - s0), -1, 1).astype(f32)
            signed = score * order
            ge_sum = None
            for h in range(heads):
                hs = slice(h * HEAD_DIM, (h + 1) * HEAD_DIM)
                gap = lcol[ts, h : h + 1] - lrow[h : h + 1, ss]
                decay = jnp.exp2(-jnp.abs(gap))
                g = jnp.dot(dyh[h, ts, :], vt[hs, ss], preferred_element_type=f32)
                ge = g * decay
                ge_sum = ge if ge_sum is None else ge_sum + ge
                se = (score * decay).astype(bf16)
                dvt[hs, ss] += jnp.dot(dyt[hs, ts], se, preferred_element_type=f32)
                pair = signed * ge
                colsum[h : h + 1, ss] += jnp.sum(pair, axis=0, keepdims=True)
                part = pair[:, :LANES]
                for piece in range(1, tile // LANES):
                    part = part + pair[:, piece * LANES : (piece + 1) * LANES]
                rowacc[h] += part
            ge_b = ge_sum.astype(bf16)
            dr[ts, :] += jnp.dot(ge_b, kn[ss, :], preferred_element_type=f32)
            dkt[:, ss] += jnp.dot(reads_t, ge_b, preferred_element_type=f32)

        for h in range(heads):
            rowdl[ts, h : h + 1] = -jnp.sum(rowacc[h], axis=1, keepdims=True)

    def finish(i, carry):
        r0 = pl.multiple_of((chunks - 1 - i) * BLOCK, BLOCK)
        rows = pl.ds(r0, BLOCK)
        into = pl.ds(pl.multiple_of(r0 + HALO, HALO), BLOCK)
        dlevel = rowdl[rows, :] + colsum[:, rows].T
        drate = jnp.dot(upper, dlevel, precision=highest, preferred_element_type=f32) + carry
        dv = dvt[:, rows].T
        u = u_ref[rows, :]
        udv = u * dv
        lane = lax.broadcasted_iota(jnp.int32, (BLOCK, LANES), 1)
        ddt = drate * fade
        for h in range(heads):
            along = jnp.sum(jnp.where(lane_head == h, udv, 0.0), axis=1, keepdims=True)
            ddt = ddt + jnp.where(lane == h, along, 0.0)
        out_ref[rows, xw + 2 * STATE :] = (ddt * sig_ref[rows, :]).astype(bf16)
        du = dv * spread(dtc_ref[rows, :]) + skip * p2_ref[rows, :xw].astype(f32)
        pad_x[into, :] = du * sux_ref[rows, :]
        sbc = sbc_ref[rows, :]
        pad_bc[into, :STATE] = dkt[:, rows].T * sbc[:, :STATE]
        pad_bc[into, STATE:] = dr[rows, :] * sbc[:, STATE:]
        return carry + jnp.sum(dlevel, axis=0, keepdims=True)

    lax.fori_loop(0, chunks, finish, jnp.zeros((1, LANES), f32))

    @pl.loop(0, chunks)
    def _(c):
        r0 = pl.multiple_of(c * BLOCK, BLOCK)
        rows = pl.ds(r0, BLOCK)
        out_ref[rows, :xw] = window_conv(pad_x, r0, tapx, True).astype(bf16)
        out_ref[rows, xw : xw + 2 * STATE] = window_conv(pad_bc, r0, tapbc, True).astype(bf16)


def mixer_backward(p1, p2, drop, tapx, tapbc, par, heads):
    window = p1.shape[0]
    xw = tapx.shape[1]
    tile = 2 * BLOCK if window % (2 * BLOCK) == 0 else BLOCK
    rows_h = -(-heads // 8) * 8
    scratch = [
        pltpu.VMEM((window + 2 * HALO, xw), f32),
        pltpu.VMEM((window + 2 * HALO, 2 * STATE), f32),
        pltpu.VMEM((window, xw), f32),
        pltpu.VMEM((window, xw), f32),
        pltpu.VMEM((window, 2 * STATE), f32),
        pltpu.VMEM((window, LANES), f32),
        pltpu.VMEM((window, LANES), f32),
        pltpu.VMEM((window, LANES), f32),
        pltpu.VMEM((rows_h, window), f32),
        pltpu.VMEM((STATE, window), bf16),
        pltpu.VMEM((STATE, window), bf16),
        pltpu.VMEM((window, STATE), bf16),
        pltpu.VMEM((window, STATE), bf16),
        pltpu.VMEM((xw, window), bf16),
        pltpu.VMEM((xw, window), bf16),
        pltpu.VMEM((heads, window, HEAD_DIM), bf16),
        pltpu.VMEM((xw, window), f32),
        pltpu.VMEM((STATE, window), f32),
        pltpu.VMEM((window, STATE), f32),
        pltpu.VMEM((heads, tile, LANES), f32),
        pltpu.VMEM((window, LANES), f32),
        pltpu.VMEM((LANES, window), f32),
    ]
    return pl.pallas_call(
        functools.partial(mixer_kernel, heads, tile),
        in_specs=[pl.BlockSpec(memory_space=pltpu.VMEM)] * 6,
        out_specs=pl.BlockSpec(memory_space=pltpu.VMEM),
        out_shape=jax.ShapeDtypeStruct((window, xw + 2 * STATE + LANES), bf16),
        scratch_shapes=scratch,
        compiler_params=pltpu.CompilerParams(vmem_limit_bytes=62 * 1024 * 1024),
        name="mixer_backward",
    )(p1, p2, drop, tapx, tapbc, par)


def pad_last(values, width):
    pads = [(0, 0)] * (values.ndim - 1) + [(0, width - values.shape[-1])]
    return jnp.pad(values, pads)


def exchange(values, axis):
    return lax.all_to_all(values, axis, split_axis=0, concat_axis=0, tiled=True)


def by_owner(values, owners):
    tokens, width = values.shape
    return jnp.transpose(values.reshape(tokens, owners, width // owners), (1, 0, 2))


def local(
    layer_activity,
    writer_matrix,
    reader_matrix,
    source_unfiltered,
    switch_raw_signal,
    saved_result,
    final_adjoint,
    delta_raw,
    extra_logdrop,
    source_filter_coefs,
    writer_filter_coefs,
    reader_filter_coefs,
    delta_offset,
    fading_exponents,
    direct_factor,
    rescale_factor,
):
    tokens = layer_activity.shape[1]
    width_in = layer_activity.shape[2]
    latent = GROUPS * STATE
    dp = lax.axis_size("dp")
    sp = lax.axis_size("sp")
    heads = delta_offset.shape[0]
    per_group = HEADS // GROUPS
    xc = heads * HEAD_DIM
    xw = -(-xc // LANES) * LANES
    window = tokens * sp

    columns = exchange(by_owner(layer_activity.reshape(tokens, width_in), dp), "dp")
    columns = columns.reshape(dp * tokens, width_in // dp)
    weights = jnp.concatenate([writer_matrix, reader_matrix], axis=1)
    partial = jnp.dot(columns, weights, preferred_element_type=f32).astype(bf16)
    p1 = exchange(
        jnp.concatenate(
            [
                pad_last(by_owner(source_unfiltered.reshape(tokens, INNER), sp), xw),
                pad_last(by_owner(delta_raw.reshape(tokens, HEADS), sp), LANES),
            ],
            axis=2,
        ),
        "sp",
    )
    result_adjoint, d_gate = norm_backward(
        saved_result.reshape(tokens, INNER),
        switch_raw_signal.reshape(tokens, INNER),
        final_adjoint.reshape(tokens, INNER),
        rescale_factor,
    )
    partial = exchange(partial.reshape(dp, tokens, 2 * latent), "dp")
    projected = jnp.sum(partial.astype(f32), axis=0).astype(bf16)
    maps = jnp.transpose(projected.reshape(tokens, 2, GROUPS, STATE), (2, 0, 1, 3))
    maps = jnp.broadcast_to(
        maps.reshape(GROUPS, 1, tokens, 2 * STATE), (GROUPS, sp // GROUPS, tokens, 2 * STATE)
    ).reshape(sp, tokens, 2 * STATE)
    p2 = exchange(
        jnp.concatenate([pad_last(by_owner(result_adjoint, sp), xw), maps], axis=2), "sp"
    )

    group = lax.axis_index("sp") * heads // per_group
    tapbc = jnp.concatenate(
        [
            lax.dynamic_slice_in_dim(writer_filter_coefs, group * STATE, STATE, axis=1),
            lax.dynamic_slice_in_dim(reader_filter_coefs, group * STATE, STATE, axis=1),
        ],
        axis=1,
    )
    par = pad_last(jnp.stack([delta_offset, jnp.exp(fading_exponents)]), LANES)
    back = mixer_backward(
        p1.reshape(window, xw + LANES),
        p2.reshape(window, xw + 2 * STATE),
        pad_last(extra_logdrop.reshape(window, heads), LANES),
        pad_last(
            jnp.concatenate([source_filter_coefs, jnp.repeat(direct_factor, HEAD_DIM)[None]]), xw
        ),
        tapbc,
        par,
        heads,
    )
    back = exchange(back.reshape(sp, tokens, xw + 2 * STATE + LANES), "sp")
    back_x = jnp.transpose(back[:, :, :xc], (1, 0, 2)).reshape(1, tokens, INNER)
    back_dt = jnp.transpose(
        back[:, :, xw + 2 * STATE : xw + 2 * STATE + heads], (1, 0, 2)
    ).reshape(1, tokens, HEADS)
    summed = jnp.sum(
        back[:, :, xw : xw + 2 * STATE]
        .astype(f32)
        .reshape(GROUPS, sp // GROUPS, tokens, 2, STATE),
        axis=1,
    )
    gradients = jnp.transpose(summed, (1, 2, 0, 3)).reshape(tokens, 2 * latent).astype(bf16)
    all_grads = exchange(
        jnp.broadcast_to(gradients[None], (dp, tokens, 2 * latent)), "dp"
    ).reshape(dp * tokens, 2 * latent)
    rows = width_in // dp
    local_rows = jnp.einsum("td,tc->dc", columns, all_grads, preferred_element_type=f32)
    shares = exchange(local_rows.astype(bf16).reshape(sp, rows // sp, 2 * latent), "sp")
    share = jnp.sum(shares.astype(f32), axis=0).astype(bf16)
    total_grad = exchange(
        jnp.broadcast_to(share[None], (sp, rows // sp, 2 * latent)), "sp"
    ).reshape(rows, 2 * latent)
    d_cols = jnp.einsum("tc,dc->td", all_grads, weights, preferred_element_type=f32)
    d_hidden = exchange(d_cols.astype(bf16).reshape(dp, tokens, rows), "dp")
    d_hidden = jnp.transpose(d_hidden, (1, 0, 2)).reshape(1, tokens, width_in)
    return (
        d_hidden,
        back_x,
        d_gate.reshape(1, tokens, INNER),
        back_dt,
        total_grad[:, :latent].astype(f32),
        total_grad[:, latent:].astype(f32),
    )


def solution(mesh):
    in_specs = (
        P("dp", "sp", None),
        P("dp", None),
        P("dp", None),
        P("dp", "sp", None),
        P("dp", "sp", None),
        P("dp", "sp", None),
        P("dp", "sp", None),
        P("dp", "sp", None),
        P("dp", None, "sp"),
        P(None, "sp"),
        P(),
        P(),
        P("sp"),
        P("sp"),
        P("sp"),
        P(),
    )
    out_specs = (
        P("dp", "sp", None),
        P("dp", "sp", None),
        P("dp", "sp", None),
        P("dp", "sp", None),
        P("dp", None),
        P("dp", None),
    )
    return jax.shard_map(local, mesh=mesh, in_specs=in_specs, out_specs=out_specs, check_vma=False)
```

```python
import functools

import jax
import jax.numpy as jnp
from jax import lax
from jax.experimental import pallas as pl
from jax.experimental.pallas import tpu as pltpu
from jax.sharding import PartitionSpec as P

HEADS = 32
HEAD_DIM = 64
STATE = 128
GROUPS = 2
NORM_GROUPS = 8
CONV_K = 5
BLOCK = 128
INNER = 2048
LANES = 128
DT_ROWS = 16
HALO = 8
EPSILON = 1e-06
LOG2E = 1.4426950408889634
highest = lax.Precision.HIGHEST
f32 = jnp.float32
bf16 = jnp.bfloat16


def sigmoid(v):
    return 1.0 / (1.0 + jnp.exp(-v))


def softplus(v):
    e = jnp.exp(-jnp.abs(v))
    z = e / (2.0 + e)
    z2 = z * z
    series = jnp.full_like(z, 1.0 / 17.0)
    for odd in (15, 13, 11, 9, 7, 5, 3, 1):
        series = series * z2 + 1.0 / odd
    return jnp.maximum(v, 0.0) + 2.0 * z * series


def window_conv(padded, r0, taps, flip):
    rows = padded[pl.ds(r0, BLOCK + 2 * HALO), :]
    total = None
    for k in range(CONV_K):
        shift = HALO - CONV_K // 2 + k
        tap = taps[CONV_K - 1 - k if flip else k][None, :]
        term = tap * pltpu.roll(rows, rows.shape[0] - shift, axis=0)[:BLOCK]
        total = term if total is None else total + term
    return total


def mixer_kernel(
    heads,
    tile,
    x_ref,
    dt_ref,
    dy_ref,
    bc_ref,
    drop_ref,
    tapx_ref,
    tapbc_ref,
    par_ref,
    dx_ref,
    dbc_ref,
    ddt_ref,
    pad_x,
    pad_bc,
    u_ref,
    sux_ref,
    sbc_ref,
    dtc_ref,
    sig_ref,
    lcol,
    lrow,
    kt,
    rt,
    kn,
    rn,
    vt,
    dyt,
    dyh,
    dvt,
    dkt,
    dr,
    rowacc,
    rowdl,
    colsum,
):
    window = x_ref.shape[0]
    xw = u_ref.shape[1]
    chunks = window // BLOCK
    tapx = tapx_ref[...]
    tapbc = tapbc_ref[...]
    offset = par_ref[0:1, :]
    fade = par_ref[1:2, :]
    skip = tapx[CONV_K : CONV_K + 1]
    lane_head = lax.broadcasted_iota(jnp.int32, (BLOCK, xw), 1) // HEAD_DIM
    row_i = lax.broadcasted_iota(jnp.int32, (BLOCK, BLOCK), 0)
    col_i = lax.broadcasted_iota(jnp.int32, (BLOCK, BLOCK), 1)
    lower = (row_i >= col_i).astype(f32)
    upper = (row_i <= col_i).astype(f32)

    def spread(columns):
        out = jnp.zeros((BLOCK, xw), f32)
        for h in range(heads):
            out = jnp.where(lane_head == h, columns[:, h : h + 1], out)
        return out

    for padded in (pad_x, pad_bc):
        padded[0:HALO, :] = jnp.zeros((HALO, padded.shape[1]), f32)
        padded[HALO + window :, :] = jnp.zeros((HALO, padded.shape[1]), f32)

    @pl.loop(0, chunks)
    def _(c):
        r0 = pl.multiple_of(c * BLOCK, BLOCK)
        rows = pl.ds(r0, BLOCK)
        into = pl.ds(pl.multiple_of(r0 + HALO, HALO), BLOCK)
        pad_x[into, :] = x_ref[rows, :].astype(f32)
        pad_bc[into, :] = bc_ref[rows, :].astype(f32)

    def prepare(c, carry):
        r0 = pl.multiple_of(c * BLOCK, BLOCK)
        rows = pl.ds(r0, BLOCK)
        steps = dt_ref[c].astype(f32)
        steps = jnp.concatenate([steps, jnp.zeros((LANES - DT_ROWS, BLOCK), f32)]).T
        a = steps + offset
        dt = softplus(a)
        dtc_ref[rows, :] = dt
        sig_ref[rows, :] = sigmoid(a)
        rate = dt * fade + drop_ref[rows, :]
        level = jnp.dot(lower, rate, precision=highest, preferred_element_type=f32) + carry
        scaled = level * LOG2E
        lcol[rows, :] = scaled
        lrow[:, rows] = scaled.T[: lrow.shape[0]]
        pre = window_conv(pad_x, r0, tapx, False)
        sig = sigmoid(pre)
        u = pre * sig
        u_ref[rows, :] = u
        sux_ref[rows, :] = sig + u * (1.0 - sig)
        vt[:, rows] = (u * spread(dt)).T.astype(bf16)
        dy_t = dy_ref[rows, :].astype(f32).T
        dyt[:, rows] = dy_t.astype(bf16)
        for h in range(heads):
            dyh[h, rows, :] = dy_t[h * HEAD_DIM : (h + 1) * HEAD_DIM].T.astype(bf16)
        pre = window_conv(pad_bc, r0, tapbc, False)
        sig = sigmoid(pre)
        kr = pre * sig
        sbc_ref[rows, :] = sig + kr * (1.0 - sig)
        kn[rows, :] = kr[:, :STATE].astype(bf16)
        rn[rows, :] = kr[:, STATE:].astype(bf16)
        kt[:, rows] = kr[:, :STATE].T.astype(bf16)
        rt[:, rows] = kr[:, STATE:].T.astype(bf16)
        return level[BLOCK - 1 : BLOCK]

    lax.fori_loop(0, chunks, prepare, jnp.zeros((1, LANES), f32))

    dvt[...] = jnp.zeros_like(dvt)
    dkt[...] = jnp.zeros_like(dkt)
    colsum[...] = jnp.zeros_like(colsum)
    rowdl[...] = jnp.zeros_like(rowdl)
    ahead = lax.broadcasted_iota(jnp.int32, (tile, tile), 0) - lax.broadcasted_iota(
        jnp.int32, (tile, tile), 1
    )

    @pl.loop(0, window // tile)
    def _(ti):
        t0 = pl.multiple_of(ti * tile, tile)
        ts = pl.ds(t0, tile)
        rowacc[...] = jnp.zeros_like(rowacc)
        dr[ts, :] = jnp.zeros((tile, STATE), f32)
        reads = rn[ts, :]
        reads_t = rt[:, ts]

        @pl.loop(0, window // tile)
        def _(si):
            s0 = pl.multiple_of(si * tile, tile)
            ss = pl.ds(s0, tile)
            score = jnp.dot(reads, kt[:, ss], preferred_element_type=f32)
            order = jnp.clip(ahead + (t0 - s0), -1, 1).astype(f32)
            signed = score * order
            ge_sum = None
            for h in range(heads):
                hs = slice(h * HEAD_DIM, (h + 1) * HEAD_DIM)
                gap = lcol[ts, h : h + 1] - lrow[h : h + 1, ss]
                decay = jnp.exp2(-jnp.abs(gap))
                g = jnp.dot(dyh[h, ts, :], vt[hs, ss], preferred_element_type=f32)
                ge = g * decay
                ge_sum = ge if ge_sum is None else ge_sum + ge
                se = (score * decay).astype(bf16)
                dvt[hs, ss] += jnp.dot(dyt[hs, ts], se, preferred_element_type=f32)
                pair = signed * ge
                colsum[h : h + 1, ss] += jnp.sum(pair, axis=0, keepdims=True)
                part = pair[:, :LANES]
                for piece in range(1, tile // LANES):
                    part = part + pair[:, piece * LANES : (piece + 1) * LANES]
                rowacc[h] += part
            ge_b = ge_sum.astype(bf16)
            dr[ts, :] += jnp.dot(ge_b, kn[ss, :], preferred_element_type=f32)
            dkt[:, ss] += jnp.dot(reads_t, ge_b, preferred_element_type=f32)

        for h in range(heads):
            rowdl[ts, h : h + 1] = -jnp.sum(rowacc[h], axis=1, keepdims=True)

    def finish(i, carry):
        r0 = pl.multiple_of((chunks - 1 - i) * BLOCK, BLOCK)
        rows = pl.ds(r0, BLOCK)
        into = pl.ds(pl.multiple_of(r0 + HALO, HALO), BLOCK)
        dlevel = rowdl[rows, :] + colsum[:, rows].T
        drate = jnp.dot(upper, dlevel, precision=highest, preferred_element_type=f32) + carry
        dv = dvt[:, rows].T
        u = u_ref[rows, :]
        udv = u * dv
        lane = lax.broadcasted_iota(jnp.int32, (BLOCK, LANES), 1)
        ddt = drate * fade
        for h in range(heads):
            along = jnp.sum(jnp.where(lane_head == h, udv, 0.0), axis=1, keepdims=True)
            ddt = ddt + jnp.where(lane == h, along, 0.0)
        ddt_ref[chunks - 1 - i] = (ddt * sig_ref[rows, :]).T[:DT_ROWS].astype(bf16)
        du = dv * spread(dtc_ref[rows, :]) + skip * dy_ref[rows, :].astype(f32)
        pad_x[into, :] = du * sux_ref[rows, :]
        sbc = sbc_ref[rows, :]
        pad_bc[into, :STATE] = dkt[:, rows].T * sbc[:, :STATE]
        pad_bc[into, STATE:] = dr[rows, :] * sbc[:, STATE:]
        return carry + jnp.sum(dlevel, axis=0, keepdims=True)

    lax.fori_loop(0, chunks, finish, jnp.zeros((1, LANES), f32))

    @pl.loop(0, chunks)
    def _(c):
        r0 = pl.multiple_of(c * BLOCK, BLOCK)
        rows = pl.ds(r0, BLOCK)
        dx_ref[rows, :] = window_conv(pad_x, r0, tapx, True).astype(bf16)
        dbc_ref[rows, :] = window_conv(pad_bc, r0, tapbc, True).astype(bf16)


def mixer_backward(x, dt, dy, bc, drop, tapx, tapbc, par, heads):
    window = x.shape[0]
    xw = tapx.shape[1]
    tile = 2 * BLOCK if window % (2 * BLOCK) == 0 else BLOCK
    rows_h = -(-heads // 8) * 8
    scratch = [
        pltpu.VMEM((window + 2 * HALO, xw), f32),
        pltpu.VMEM((window + 2 * HALO, 2 * STATE), f32),
        pltpu.VMEM((window, xw), f32),
        pltpu.VMEM((window, xw), f32),
        pltpu.VMEM((window, 2 * STATE), f32),
        pltpu.VMEM((window, LANES), f32),
        pltpu.VMEM((window, LANES), f32),
        pltpu.VMEM((window, LANES), f32),
        pltpu.VMEM((rows_h, window), f32),
        pltpu.VMEM((STATE, window), bf16),
        pltpu.VMEM((STATE, window), bf16),
        pltpu.VMEM((window, STATE), bf16),
        pltpu.VMEM((window, STATE), bf16),
        pltpu.VMEM((xw, window), bf16),
        pltpu.VMEM((xw, window), bf16),
        pltpu.VMEM((heads, window, HEAD_DIM), bf16),
        pltpu.VMEM((xw, window), f32),
        pltpu.VMEM((STATE, window), f32),
        pltpu.VMEM((window, STATE), f32),
        pltpu.VMEM((heads, tile, LANES), f32),
        pltpu.VMEM((window, LANES), f32),
        pltpu.VMEM((LANES, window), f32),
    ]
    return pl.pallas_call(
        functools.partial(mixer_kernel, heads, tile),
        in_specs=[pl.BlockSpec(memory_space=pltpu.VMEM)] * 8,
        out_specs=[pl.BlockSpec(memory_space=pltpu.VMEM)] * 3,
        out_shape=[
            jax.ShapeDtypeStruct((window, xw), bf16),
            jax.ShapeDtypeStruct((window, 2 * STATE), bf16),
            jax.ShapeDtypeStruct(dt.shape, bf16),
        ],
        scratch_shapes=scratch,
        compiler_params=pltpu.CompilerParams(vmem_limit_bytes=62 * 1024 * 1024),
        name="mixer_backward",
    )(x, dt, dy, bc, drop, tapx, tapbc, par)


def pad_last(values, width):
    pads = [(0, 0)] * (values.ndim - 1) + [(0, width - values.shape[-1])]
    return jnp.pad(values, pads)


def by_owner(values, owners):
    tokens, width = values.shape
    return jnp.transpose(values.reshape(tokens, owners, width // owners), (1, 0, 2))


def greet(axes):
    barrier = pltpu.get_barrier_semaphore()
    count = 0
    for axis in axes:
        size = lax.axis_size(axis)
        me = lax.axis_index(axis)
        for o in range(1, size):
            pl.semaphore_signal(
                barrier,
                inc=1,
                device_id={axis: lax.rem(me + o, size)},
                device_id_type=pl.DeviceIdType.MESH,
            )
            count += 1
    pl.semaphore_wait(barrier, count)


def send_all(axis, source, target, sems, slot):
    size = lax.axis_size(axis)
    me = lax.axis_index(axis)
    copies = []
    for o in range(1, size):
        peer = lax.rem(me + o, size)
        copies.append(
            pltpu.make_async_remote_copy(
                src_ref=source(peer),
                dst_ref=target(me),
                send_sem=sems.at[slot, 0, o],
                recv_sem=sems.at[slot, 1, o],
                device_id={axis: peer},
                device_id_type=pl.DeviceIdType.MESH,
            )
        )
    for copy in copies:
        copy.start()
    return copies


def received(copies):
    for copy in copies:
        copy.wait_recv()


def lanes_of(index, width):
    return pl.ds(pl.multiple_of(index * width, LANES), width)


def front_kernel(
    heads,
    la_ref,
    w_ref,
    x_ref,
    dt_ref,
    values_ref,
    gates_ref,
    adjoint_ref,
    scale_ref,
    cols_ref,
    xall_ref,
    dtall_ref,
    dyall_ref,
    bcall_ref,
    dgate_ref,
    dysend,
    psend,
    pall,
    bcsend,
    sems,
):
    dp = lax.axis_size("dp")
    sp = lax.axis_size("sp")
    me_dp = lax.axis_index("dp")
    me_sp = lax.axis_index("sp")
    tokens, width_in = la_ref.shape
    cw = width_in // dp
    xc = heads * HEAD_DIM
    per_group = HEADS // GROUPS
    greet(("dp", "sp"))
    la_copies = send_all(
        "dp", lambda p: la_ref.at[:, lanes_of(p, cw)], lambda m: cols_ref.at[m], sems, 0
    )
    x_copies = send_all("sp", lambda p: x_ref.at[p], lambda m: xall_ref.at[m], sems, 1)
    dt_copies = send_all("sp", lambda p: dt_ref.at[p], lambda m: dtall_ref.at[m], sems, 2)
    cols_ref[me_dp] = la_ref[:, lanes_of(me_dp, cw)]
    xall_ref[me_sp] = x_ref[me_sp]
    dtall_ref[me_sp] = dt_ref[me_sp]

    inner = values_ref.shape[1]
    width = inner // NORM_GROUPS
    for group in range(NORM_GROUPS):
        span = slice(group * width, (group + 1) * width)
        values = values_ref[:, span].astype(f32)
        gates = gates_ref[:, span].astype(f32)
        sig = sigmoid(gates)
        act = gates * sig
        g = values * act
        dn = adjoint_ref[:, span].astype(f32) * scale_ref[:, span]
        inv = lax.rsqrt(jnp.sum(g * g, axis=1, keepdims=True) * (1.0 / width) + EPSILON)
        along = jnp.sum(dn * g, axis=1, keepdims=True) * (1.0 / width)
        dg = inv * dn - g * (inv * inv * inv * along)
        dgate_ref[:, span] = (dg * values * (sig + act * (1.0 - sig))).astype(bf16)
        dy = (dg * act).astype(bf16)
        step = min(width, xc)
        for part in range(width // step):
            at = group * width + part * step
            owner, first = at // xc, at % xc
            dysend[owner, :, first : first + step] = dy[:, part * step : (part + 1) * step]
            if xc < dysend.shape[2]:
                dysend[owner, :, xc:] = jnp.zeros((tokens, dysend.shape[2] - xc), bf16)
    dy_copies = send_all("sp", lambda p: dysend.at[p], lambda m: dyall_ref.at[m], sems, 3)
    dyall_ref[me_sp] = dysend[me_sp]

    received(la_copies)
    for i in range(dp):
        psend[i] = jnp.dot(cols_ref[i], w_ref[...], preferred_element_type=f32).astype(bf16)
    p_copies = send_all("dp", lambda p: psend.at[p], lambda m: pall.at[m], sems, 4)
    total = psend[me_dp].astype(f32)
    pall[me_dp] = jnp.zeros(pall.shape[1:], bf16)
    received(p_copies)
    for i in range(dp):
        total = total + pall[i].astype(f32)
    total = total.astype(bf16)
    for group in range(GROUPS):
        at = group * STATE
        bcsend[group, :, :STATE] = total[:, at : at + STATE]
        at = (GROUPS + group) * STATE
        bcsend[group, :, STATE:] = total[:, at : at + STATE]
    bc_copies = send_all(
        "sp",
        lambda p: bcsend.at[(p * heads) // per_group],
        lambda m: bcall_ref.at[m],
        sems,
        5,
    )
    bcall_ref[me_sp] = bcsend[(me_sp * heads) // per_group]
    for copies in (x_copies, dt_copies, dy_copies, bc_copies):
        received(copies)
    for copies in (la_copies, x_copies, dt_copies, dy_copies, p_copies, bc_copies):
        for copy in copies:
            copy.wait_send()


def back_kernel(
    heads,
    dx_ref,
    dbc_ref,
    ddt_ref,
    cols_ref,
    w_ref,
    dxout_ref,
    ddtout_ref,
    dh_ref,
    dwb_ref,
    dwc_ref,
    dbcall,
    gall,
    gsend,
    wsend,
    wall,
    hsend,
    ssend,
    tall,
    sems,
):
    dp = lax.axis_size("dp")
    sp = lax.axis_size("sp")
    me_dp = lax.axis_index("dp")
    me_sp = lax.axis_index("sp")
    tokens = dx_ref.shape[1]
    cw = w_ref.shape[0]
    xc = heads * HEAD_DIM
    latent = GROUPS * STATE
    direct = xc % LANES == 0
    rows = cw // sp
    greet(("dp", "sp"))
    dbc_copies = send_all("sp", lambda p: dbc_ref.at[p], lambda m: dbcall.at[m], sems, 0)
    if direct:
        dx_to = lambda m: dxout_ref.at[:, lanes_of(m, xc)]
    else:
        dx_to = lambda m: dxout_ref.at[m]
    dx_copies = send_all("sp", lambda p: dx_ref.at[p], dx_to, sems, 1)
    ddt_copies = send_all("sp", lambda p: ddt_ref.at[p], lambda m: ddtout_ref.at[m], sems, 2)
    dbcall[me_sp] = dbc_ref[me_sp]
    ddtout_ref[me_sp] = ddt_ref[me_sp]
    if direct:
        dxout_ref[:, lanes_of(me_sp, xc)] = dx_ref[me_sp]
    else:
        dxout_ref[me_sp] = dx_ref[me_sp]
    received(dbc_copies)
    members = sp // GROUPS
    for group in range(GROUPS):
        total = dbcall[group * members].astype(f32)
        for member in range(1, members):
            total = total + dbcall[group * members + member].astype(f32)
        total = total.astype(bf16)
        at = group * STATE
        gsend[:, at : at + STATE] = total[:, :STATE]
        at = (GROUPS + group) * STATE
        gsend[:, at : at + STATE] = total[:, STATE:]
    g_copies = send_all("dp", lambda p: gsend, lambda m: gall.at[m], sems, 3)
    gall[me_dp] = gsend[...]
    received(g_copies)
    total = None
    for i in range(dp):
        term = lax.dot_general(
            cols_ref[i], gall[i], (((0,), (0,)), ((), ())), preferred_element_type=f32
        )
        total = term if total is None else total + term
    wsend[...] = total.astype(bf16).reshape(sp, rows, 2 * latent)
    w_copies = send_all("sp", lambda p: wsend.at[p], lambda m: wall.at[m], sems, 4)
    wall[me_sp] = wsend[me_sp]
    for i in range(dp):
        hsend[i] = lax.dot_general(
            gall[i], w_ref[...], (((1,), (1,)), ((), ())), preferred_element_type=f32
        ).astype(bf16)
    h_copies = send_all(
        "dp", lambda p: hsend.at[p], lambda m: dh_ref.at[:, lanes_of(m, cw)], sems, 5
    )
    dh_ref[:, lanes_of(me_dp, cw)] = hsend[me_dp]
    received(w_copies)
    share = wall[0].astype(f32)
    for j in range(1, sp):
        share = share + wall[j].astype(f32)
    ssend[...] = share.astype(bf16)
    s_copies = send_all("sp", lambda p: ssend, lambda m: tall.at[m], sems, 6)
    tall[me_sp] = ssend[...]
    received(s_copies)
    for j in range(sp):
        dwb_ref[j] = tall[j, :, :latent].astype(f32)
        dwc_ref[j] = tall[j, :, latent:].astype(f32)
    for copies in (dx_copies, ddt_copies, h_copies):
        received(copies)
    for copies in (
        dbc_copies,
        dx_copies,
        ddt_copies,
        g_copies,
        w_copies,
        h_copies,
        s_copies,
    ):
        for copy in copies:
            copy.wait_send()


def comm_call(kernel, args, shapes, scratch, slots, peers, number, name):
    vmem = pl.BlockSpec(memory_space=pltpu.VMEM)
    return pl.pallas_call(
        kernel,
        in_specs=[vmem] * len(args),
        out_specs=[vmem] * len(shapes),
        out_shape=[jax.ShapeDtypeStruct(shape, kind) for shape, kind in shapes],
        scratch_shapes=[pltpu.VMEM(shape, bf16) for shape in scratch]
        + [pltpu.SemaphoreType.DMA((slots, 2, peers))],
        compiler_params=pltpu.CompilerParams(
            collective_id=number, has_side_effects=True, vmem_limit_bytes=60 * 1024 * 1024
        ),
        name=name,
    )(*args)


def local(
    layer_activity,
    writer_matrix,
    reader_matrix,
    source_unfiltered,
    switch_raw_signal,
    saved_result,
    final_adjoint,
    delta_raw,
    extra_logdrop,
    source_filter_coefs,
    writer_filter_coefs,
    reader_filter_coefs,
    delta_offset,
    fading_exponents,
    direct_factor,
    rescale_factor,
):
    tokens = layer_activity.shape[1]
    width_in = layer_activity.shape[2]
    latent = GROUPS * STATE
    dp = lax.axis_size("dp")
    sp = lax.axis_size("sp")
    heads = delta_offset.shape[0]
    per_group = HEADS // GROUPS
    xc = heads * HEAD_DIM
    xw = -(-xc // LANES) * LANES
    window = tokens * sp
    cw = width_in // dp
    peers = max(sp, dp)

    weights = jnp.concatenate([writer_matrix, reader_matrix], axis=1)
    x_by = pad_last(by_owner(source_unfiltered.reshape(tokens, INNER), sp), xw)
    dt_by = delta_raw.reshape(tokens, HEADS).T.reshape(sp, heads, tokens)
    dt_by = jnp.pad(dt_by, ((0, 0), (0, DT_ROWS - heads), (0, 0)))
    cols, x_all, dt_all, dy_all, bc_all, d_gate = comm_call(
        functools.partial(front_kernel, heads),
        (
            layer_activity.reshape(tokens, width_in),
            weights,
            x_by,
            dt_by,
            saved_result.reshape(tokens, INNER),
            switch_raw_signal.reshape(tokens, INNER),
            final_adjoint.reshape(tokens, INNER),
            rescale_factor.reshape(1, INNER),
        ),
        (
            ((dp, tokens, cw), bf16),
            ((sp, tokens, xw), bf16),
            ((sp, DT_ROWS, tokens), bf16),
            ((sp, tokens, xw), bf16),
            ((sp, tokens, 2 * STATE), bf16),
            ((tokens, INNER), bf16),
        ),
        (
            (sp, tokens, xw),
            (dp, tokens, 2 * latent),
            (dp, tokens, 2 * latent),
            (GROUPS, tokens, 2 * STATE),
        ),
        6,
        peers,
        0,
        "front",
    )

    group = lax.axis_index("sp") * heads // per_group
    tapbc = jnp.concatenate(
        [
            lax.dynamic_slice_in_dim(writer_filter_coefs, group * STATE, STATE, axis=1),
            lax.dynamic_slice_in_dim(reader_filter_coefs, group * STATE, STATE, axis=1),
        ],
        axis=1,
    )
    par = pad_last(jnp.stack([delta_offset, jnp.exp(fading_exponents)]), LANES)
    dx, dbc, ddt = mixer_backward(
        x_all.reshape(window, xw),
        dt_all,
        dy_all.reshape(window, xw),
        bc_all.reshape(window, 2 * STATE),
        pad_last(extra_logdrop.reshape(window, heads), LANES),
        pad_last(
            jnp.concatenate([source_filter_coefs, jnp.repeat(direct_factor, HEAD_DIM)[None]]), xw
        ),
        tapbc,
        par,
        heads,
    )
    rows = cw // sp
    back_x, back_dt, d_hidden, d_w_b, d_w_c = comm_call(
        functools.partial(back_kernel, heads),
        (
            dx.reshape(sp, tokens, xw),
            dbc.reshape(sp, tokens, 2 * STATE),
            ddt,
            cols,
            weights,
        ),
        (
            ((tokens, INNER) if xc % LANES == 0 else (sp, tokens, xw), bf16),
            ((sp, DT_ROWS, tokens), bf16),
            ((tokens, width_in), bf16),
            ((sp, rows, latent), f32),
            ((sp, rows, latent), f32),
        ),
        (
            (sp, tokens, 2 * STATE),
            (dp, tokens, 2 * latent),
            (tokens, 2 * latent),
            (sp, rows, 2 * latent),
            (sp, rows, 2 * latent),
            (dp, tokens, cw),
            (rows, 2 * latent),
            (sp, rows, 2 * latent),
        ),
        7,
        peers,
        1,
        "back",
    )
    if xc % LANES:
        back_x = jnp.transpose(back_x[:, :, :xc], (1, 0, 2))
    back_dt = back_dt[:, :heads].reshape(HEADS, tokens).T
    return (
        d_hidden.reshape(1, tokens, width_in),
        back_x.reshape(1, tokens, INNER),
        d_gate.reshape(1, tokens, INNER),
        back_dt.reshape(1, tokens, HEADS),
        d_w_b.reshape(cw, latent),
        d_w_c.reshape(cw, latent),
    )


def solution(mesh):
    in_specs = (
        P("dp", "sp", None),
        P("dp", None),
        P("dp", None),
        P("dp", "sp", None),
        P("dp", "sp", None),
        P("dp", "sp", None),
        P("dp", "sp", None),
        P("dp", "sp", None),
        P("dp", None, "sp"),
        P(None, "sp"),
        P(),
        P(),
        P("sp"),
        P("sp"),
        P("sp"),
        P(),
    )
    out_specs = (
        P("dp", "sp", None),
        P("dp", "sp", None),
        P("dp", "sp", None),
        P("dp", "sp", None),
        P("dp", None),
        P("dp", None),
    )
    return jax.shard_map(local, mesh=mesh, in_specs=in_specs, out_specs=out_specs, check_vma=False)
```

```python
import functools

import jax
import jax.numpy as jnp
from jax import lax
from jax.experimental import pallas as pl
from jax.experimental.pallas import tpu as pltpu
from jax.sharding import PartitionSpec as P

HEADS = 32
HEAD_DIM = 64
STATE = 128
GROUPS = 2
NORM_GROUPS = 8
CONV_K = 5
BLOCK = 128
INNER = 2048
LANES = 128
DT_ROWS = 16
HALO = 8
EPSILON = 1e-06
LOG2E = 1.4426950408889634
highest = lax.Precision.HIGHEST
f32 = jnp.float32
bf16 = jnp.bfloat16


def sigmoid(v):
    return 1.0 / (1.0 + jnp.exp(-v))


def softplus(v):
    e = jnp.exp(-jnp.abs(v))
    z = e / (2.0 + e)
    z2 = z * z
    series = jnp.full_like(z, 1.0 / 17.0)
    for odd in (15, 13, 11, 9, 7, 5, 3, 1):
        series = series * z2 + 1.0 / odd
    return jnp.maximum(v, 0.0) + 2.0 * z * series


def window_conv(padded, r0, taps, flip):
    rows = padded[pl.ds(r0, BLOCK + 2 * HALO), :]
    total = None
    for k in range(CONV_K):
        shift = HALO - CONV_K // 2 + k
        tap = taps[CONV_K - 1 - k if flip else k][None, :]
        term = tap * pltpu.roll(rows, rows.shape[0] - shift, axis=0)[:BLOCK]
        total = term if total is None else total + term
    return total


def mixer_kernel(
    heads,
    tile,
    x_ref,
    dt_ref,
    dy_ref,
    bc_ref,
    drop_ref,
    tapx_ref,
    tapbc_ref,
    par_ref,
    dx_ref,
    dbc_ref,
    ddt_ref,
    pad_x,
    pad_bc,
    u_ref,
    sux_ref,
    sbc_ref,
    dtc_ref,
    sig_ref,
    lcol,
    lrow,
    kt,
    rt,
    kn,
    rn,
    vt,
    dyt,
    dyh,
    dvt,
    dkt,
    dr,
    rowacc,
    rowdl,
    colsum,
):
    window = x_ref.shape[0]
    xw = u_ref.shape[1]
    chunks = window // BLOCK
    tapx = tapx_ref[...]
    tapbc = tapbc_ref[...]
    offset = par_ref[0:1, :]
    fade = par_ref[1:2, :]
    skip = tapx[CONV_K : CONV_K + 1]
    lane_head = lax.broadcasted_iota(jnp.int32, (BLOCK, xw), 1) // HEAD_DIM
    row_i = lax.broadcasted_iota(jnp.int32, (BLOCK, BLOCK), 0)
    col_i = lax.broadcasted_iota(jnp.int32, (BLOCK, BLOCK), 1)
    lower = (row_i >= col_i).astype(f32)
    upper = (row_i <= col_i).astype(f32)

    def spread(columns):
        out = jnp.zeros((BLOCK, xw), f32)
        for h in range(heads):
            out = jnp.where(lane_head == h, columns[:, h : h + 1], out)
        return out

    for padded in (pad_x, pad_bc):
        padded[0:HALO, :] = jnp.zeros((HALO, padded.shape[1]), f32)
        padded[HALO + window :, :] = jnp.zeros((HALO, padded.shape[1]), f32)

    @pl.loop(0, chunks)
    def _(c):
        r0 = pl.multiple_of(c * BLOCK, BLOCK)
        rows = pl.ds(r0, BLOCK)
        into = pl.ds(pl.multiple_of(r0 + HALO, HALO), BLOCK)
        pad_x[into, :] = x_ref[rows, :].astype(f32)
        pad_bc[into, :] = bc_ref[rows, :].astype(f32)

    def prepare(c, carry):
        r0 = pl.multiple_of(c * BLOCK, BLOCK)
        rows = pl.ds(r0, BLOCK)
        steps = dt_ref[c].astype(f32)
        steps = jnp.concatenate([steps, jnp.zeros((LANES - DT_ROWS, BLOCK), f32)]).T
        a = steps + offset
        dt = softplus(a)
        dtc_ref[rows, :] = dt
        sig_ref[rows, :] = sigmoid(a)
        rate = dt * fade + drop_ref[rows, :]
        level = jnp.dot(lower, rate, precision=highest, preferred_element_type=f32) + carry
        scaled = level * LOG2E
        lcol[rows, :] = scaled
        lrow[:, rows] = scaled.T[: lrow.shape[0]]
        pre = window_conv(pad_x, r0, tapx, False)
        sig = sigmoid(pre)
        u = pre * sig
        u_ref[rows, :] = u
        sux_ref[rows, :] = sig + u * (1.0 - sig)
        vt[:, rows] = (u * spread(dt)).T.astype(bf16)
        dy_t = dy_ref[rows, :].astype(f32).T
        dyt[:, rows] = dy_t.astype(bf16)
        for h in range(heads):
            dyh[h, rows, :] = dy_t[h * HEAD_DIM : (h + 1) * HEAD_DIM].T.astype(bf16)
        pre = window_conv(pad_bc, r0, tapbc, False)
        sig = sigmoid(pre)
        kr = pre * sig
        sbc_ref[rows, :] = sig + kr * (1.0 - sig)
        kn[rows, :] = kr[:, :STATE].astype(bf16)
        rn[rows, :] = kr[:, STATE:].astype(bf16)
        kt[:, rows] = kr[:, :STATE].T.astype(bf16)
        rt[:, rows] = kr[:, STATE:].T.astype(bf16)
        return level[BLOCK - 1 : BLOCK]

    lax.fori_loop(0, chunks, prepare, jnp.zeros((1, LANES), f32))

    dvt[...] = jnp.zeros_like(dvt)
    dkt[...] = jnp.zeros_like(dkt)
    colsum[...] = jnp.zeros_like(colsum)
    rowdl[...] = jnp.zeros_like(rowdl)
    ahead = lax.broadcasted_iota(jnp.int32, (tile, tile), 0) - lax.broadcasted_iota(
        jnp.int32, (tile, tile), 1
    )

    @pl.loop(0, window // tile)
    def _(ti):
        t0 = pl.multiple_of(ti * tile, tile)
        ts = pl.ds(t0, tile)
        rowacc[...] = jnp.zeros_like(rowacc)
        dr[ts, :] = jnp.zeros((tile, STATE), f32)
        reads = rn[ts, :]
        reads_t = rt[:, ts]

        @pl.loop(0, window // tile)
        def _(si):
            s0 = pl.multiple_of(si * tile, tile)
            ss = pl.ds(s0, tile)
            score = jnp.dot(reads, kt[:, ss], preferred_element_type=f32)
            order = jnp.clip(ahead + (t0 - s0), -1, 1).astype(f32)
            signed = score * order
            ge_sum = None
            for h in range(heads):
                hs = slice(h * HEAD_DIM, (h + 1) * HEAD_DIM)
                gap = lcol[ts, h : h + 1] - lrow[h : h + 1, ss]
                decay = jnp.exp2(-jnp.abs(gap))
                g = jnp.dot(dyh[h, ts, :], vt[hs, ss], preferred_element_type=f32)
                ge = g * decay
                ge_sum = ge if ge_sum is None else ge_sum + ge
                se = (score * decay).astype(bf16)
                dvt[hs, ss] += jnp.dot(dyt[hs, ts], se, preferred_element_type=f32)
                pair = signed * ge
                colsum[h : h + 1, ss] += jnp.sum(pair, axis=0, keepdims=True)
                part = pair[:, :LANES]
                for piece in range(1, tile // LANES):
                    part = part + pair[:, piece * LANES : (piece + 1) * LANES]
                rowacc[h] += part
            ge_b = ge_sum.astype(bf16)
            dr[ts, :] += jnp.dot(ge_b, kn[ss, :], preferred_element_type=f32)
            dkt[:, ss] += jnp.dot(reads_t, ge_b, preferred_element_type=f32)

        for h in range(heads):
            rowdl[ts, h : h + 1] = -jnp.sum(rowacc[h], axis=1, keepdims=True)

    def finish(i, carry):
        r0 = pl.multiple_of((chunks - 1 - i) * BLOCK, BLOCK)
        rows = pl.ds(r0, BLOCK)
        into = pl.ds(pl.multiple_of(r0 + HALO, HALO), BLOCK)
        dlevel = rowdl[rows, :] + colsum[:, rows].T
        drate = jnp.dot(upper, dlevel, precision=highest, preferred_element_type=f32) + carry
        dv = dvt[:, rows].T
        u = u_ref[rows, :]
        udv = u * dv
        lane = lax.broadcasted_iota(jnp.int32, (BLOCK, LANES), 1)
        ddt = drate * fade
        for h in range(heads):
            along = jnp.sum(jnp.where(lane_head == h, udv, 0.0), axis=1, keepdims=True)
            ddt = ddt + jnp.where(lane == h, along, 0.0)
        ddt_ref[chunks - 1 - i] = (ddt * sig_ref[rows, :]).T[:DT_ROWS].astype(bf16)
        du = dv * spread(dtc_ref[rows, :]) + skip * dy_ref[rows, :].astype(f32)
        pad_x[into, :] = du * sux_ref[rows, :]
        sbc = sbc_ref[rows, :]
        pad_bc[into, :STATE] = dkt[:, rows].T * sbc[:, :STATE]
        pad_bc[into, STATE:] = dr[rows, :] * sbc[:, STATE:]
        return carry + jnp.sum(dlevel, axis=0, keepdims=True)

    lax.fori_loop(0, chunks, finish, jnp.zeros((1, LANES), f32))

    @pl.loop(0, chunks)
    def _(c):
        r0 = pl.multiple_of(c * BLOCK, BLOCK)
        rows = pl.ds(r0, BLOCK)
        dx_ref[rows, :] = window_conv(pad_x, r0, tapx, True).astype(bf16)
        dbc_ref[rows, :] = window_conv(pad_bc, r0, tapbc, True).astype(bf16)


def mixer_backward(x, dt, dy, bc, drop, tapx, tapbc, par, heads):
    window = x.shape[0]
    xw = tapx.shape[1]
    tile = 2 * BLOCK if window % (2 * BLOCK) == 0 else BLOCK
    rows_h = -(-heads // 8) * 8
    scratch = [
        pltpu.VMEM((window + 2 * HALO, xw), f32),
        pltpu.VMEM((window + 2 * HALO, 2 * STATE), f32),
        pltpu.VMEM((window, xw), f32),
        pltpu.VMEM((window, xw), f32),
        pltpu.VMEM((window, 2 * STATE), f32),
        pltpu.VMEM((window, LANES), f32),
        pltpu.VMEM((window, LANES), f32),
        pltpu.VMEM((window, LANES), f32),
        pltpu.VMEM((rows_h, window), f32),
        pltpu.VMEM((STATE, window), bf16),
        pltpu.VMEM((STATE, window), bf16),
        pltpu.VMEM((window, STATE), bf16),
        pltpu.VMEM((window, STATE), bf16),
        pltpu.VMEM((xw, window), bf16),
        pltpu.VMEM((xw, window), bf16),
        pltpu.VMEM((heads, window, HEAD_DIM), bf16),
        pltpu.VMEM((xw, window), f32),
        pltpu.VMEM((STATE, window), f32),
        pltpu.VMEM((window, STATE), f32),
        pltpu.VMEM((heads, tile, LANES), f32),
        pltpu.VMEM((window, LANES), f32),
        pltpu.VMEM((LANES, window), f32),
    ]
    return pl.pallas_call(
        functools.partial(mixer_kernel, heads, tile),
        in_specs=[pl.BlockSpec(memory_space=pltpu.VMEM)] * 8,
        out_specs=[pl.BlockSpec(memory_space=pltpu.VMEM)] * 3,
        out_shape=[
            jax.ShapeDtypeStruct((window, xw), bf16),
            jax.ShapeDtypeStruct((window, 2 * STATE), bf16),
            jax.ShapeDtypeStruct(dt.shape, bf16),
        ],
        scratch_shapes=scratch,
        compiler_params=pltpu.CompilerParams(vmem_limit_bytes=62 * 1024 * 1024),
        name="mixer_backward",
    )(x, dt, dy, bc, drop, tapx, tapbc, par)


def pad_last(values, width):
    pads = [(0, 0)] * (values.ndim - 1) + [(0, width - values.shape[-1])]
    return jnp.pad(values, pads)


def by_owner(values, owners):
    tokens, width = values.shape
    return jnp.transpose(values.reshape(tokens, owners, width // owners), (1, 0, 2))


def greet(axes):
    barrier = pltpu.get_barrier_semaphore()
    count = 0
    for axis in axes:
        size = lax.axis_size(axis)
        me = lax.axis_index(axis)
        for o in range(1, size):
            pl.semaphore_signal(
                barrier,
                inc=1,
                device_id={axis: lax.rem(me + o, size)},
                device_id_type=pl.DeviceIdType.MESH,
            )
            count += 1
    pl.semaphore_wait(barrier, count)


def send_all(axis, source, target, sems, slot):
    size = lax.axis_size(axis)
    me = lax.axis_index(axis)
    copies = []
    for o in range(1, size):
        peer = lax.rem(me + o, size)
        copies.append(
            pltpu.make_async_remote_copy(
                src_ref=source(peer),
                dst_ref=target(me),
                send_sem=sems.at[slot, 0, o],
                recv_sem=sems.at[slot, 1, o],
                device_id={axis: peer},
                device_id_type=pl.DeviceIdType.MESH,
            )
        )
    for copy in copies:
        copy.start()
    return copies


def received(copies):
    for copy in copies:
        copy.wait_recv()


def lanes_of(index, width):
    return pl.ds(pl.multiple_of(index * width, LANES), width)


def front_kernel(
    heads,
    la_ref,
    w_ref,
    x_ref,
    dt_ref,
    values_ref,
    gates_ref,
    adjoint_ref,
    scale_ref,
    cols_ref,
    xall_ref,
    dtall_ref,
    dyall_ref,
    bcall_ref,
    dgate_ref,
    dysend,
    psend,
    pall,
    bcsend,
    sems,
):
    dp = lax.axis_size("dp")
    sp = lax.axis_size("sp")
    me_dp = lax.axis_index("dp")
    me_sp = lax.axis_index("sp")
    tokens, width_in = la_ref.shape
    cw = width_in // dp
    xc = heads * HEAD_DIM
    per_group = HEADS // GROUPS
    greet(("dp", "sp"))
    la_copies = send_all(
        "dp", lambda p: la_ref.at[:, lanes_of(p, cw)], lambda m: cols_ref.at[m], sems, 0
    )
    x_copies = send_all("sp", lambda p: x_ref.at[p], lambda m: xall_ref.at[m], sems, 1)
    dt_copies = send_all("sp", lambda p: dt_ref.at[p], lambda m: dtall_ref.at[m], sems, 2)
    cols_ref[me_dp] = la_ref[:, lanes_of(me_dp, cw)]
    xall_ref[me_sp] = x_ref[me_sp]
    dtall_ref[me_sp] = dt_ref[me_sp]

    inner = values_ref.shape[1]
    width = inner // NORM_GROUPS
    for group in range(NORM_GROUPS):
        span = slice(group * width, (group + 1) * width)
        values = values_ref[:, span].astype(f32)
        gates = gates_ref[:, span].astype(f32)
        sig = sigmoid(gates)
        act = gates * sig
        g = values * act
        dn = adjoint_ref[:, span].astype(f32) * scale_ref[:, span]
        inv = lax.rsqrt(jnp.sum(g * g, axis=1, keepdims=True) * (1.0 / width) + EPSILON)
        along = jnp.sum(dn * g, axis=1, keepdims=True) * (1.0 / width)
        dg = inv * dn - g * (inv * inv * inv * along)
        dgate_ref[:, span] = (dg * values * (sig + act * (1.0 - sig))).astype(bf16)
        dy = (dg * act).astype(bf16)
        step = min(width, xc)
        for part in range(width // step):
            at = group * width + part * step
            owner, first = at // xc, at % xc
            dysend[owner, :, first : first + step] = dy[:, part * step : (part + 1) * step]
            if xc < dysend.shape[2]:
                dysend[owner, :, xc:] = jnp.zeros((tokens, dysend.shape[2] - xc), bf16)
    dy_copies = send_all("sp", lambda p: dysend.at[p], lambda m: dyall_ref.at[m], sems, 3)
    dyall_ref[me_sp] = dysend[me_sp]

    received(la_copies)
    for i in range(dp):
        psend[i] = jnp.dot(cols_ref[i], w_ref[...], preferred_element_type=f32).astype(bf16)
    p_copies = send_all("dp", lambda p: psend.at[p], lambda m: pall.at[m], sems, 4)
    total = psend[me_dp].astype(f32)
    pall[me_dp] = jnp.zeros(pall.shape[1:], bf16)
    received(p_copies)
    for i in range(dp):
        total = total + pall[i].astype(f32)
    total = total.astype(bf16)
    for group in range(GROUPS):
        at = group * STATE
        bcsend[group, :, :STATE] = total[:, at : at + STATE]
        at = (GROUPS + group) * STATE
        bcsend[group, :, STATE:] = total[:, at : at + STATE]
    bc_copies = send_all(
        "sp",
        lambda p: bcsend.at[(p * heads) // per_group],
        lambda m: bcall_ref.at[m],
        sems,
        5,
    )
    bcall_ref[me_sp] = bcsend[(me_sp * heads) // per_group]
    for copies in (x_copies, dt_copies, dy_copies, bc_copies):
        received(copies)
    for copies in (la_copies, x_copies, dt_copies, dy_copies, p_copies, bc_copies):
        for copy in copies:
            copy.wait_send()


def back_kernel(
    heads,
    dx_ref,
    dbc_ref,
    ddt_ref,
    cols_ref,
    w_ref,
    dxout_ref,
    ddtout_ref,
    dh_ref,
    dwb_ref,
    dwc_ref,
    dbcall,
    gall,
    gsend,
    wsend,
    wall,
    hsend,
    ssend,
    tall,
    sems,
):
    dp = lax.axis_size("dp")
    sp = lax.axis_size("sp")
    me_dp = lax.axis_index("dp")
    me_sp = lax.axis_index("sp")
    tokens = dx_ref.shape[1]
    cw = w_ref.shape[0]
    xc = heads * HEAD_DIM
    latent = GROUPS * STATE
    direct = xc % LANES == 0
    rows = cw // sp
    greet(("dp", "sp"))
    dbc_copies = send_all("sp", lambda p: dbc_ref.at[p], lambda m: dbcall.at[m], sems, 0)
    if direct:
        dx_to = lambda m: dxout_ref.at[:, lanes_of(m, xc)]
    else:
        dx_to = lambda m: dxout_ref.at[m]
    dbcall[me_sp] = dbc_ref[me_sp]
    ddtout_ref[me_sp] = ddt_ref[me_sp]
    if direct:
        dxout_ref[:, lanes_of(me_sp, xc)] = dx_ref[me_sp]
    else:
        dxout_ref[me_sp] = dx_ref[me_sp]
    received(dbc_copies)
    members = sp // GROUPS
    for group in range(GROUPS):
        total = dbcall[group * members].astype(f32)
        for member in range(1, members):
            total = total + dbcall[group * members + member].astype(f32)
        total = total.astype(bf16)
        at = group * STATE
        gsend[:, at : at + STATE] = total[:, :STATE]
        at = (GROUPS + group) * STATE
        gsend[:, at : at + STATE] = total[:, STATE:]
    g_copies = send_all("dp", lambda p: gsend, lambda m: gall.at[m], sems, 3)
    dx_copies = send_all("sp", lambda p: dx_ref.at[p], dx_to, sems, 1)
    ddt_copies = send_all("sp", lambda p: ddt_ref.at[p], lambda m: ddtout_ref.at[m], sems, 2)
    gall[me_dp] = gsend[...]
    received(g_copies)
    total = None
    for i in range(dp):
        term = lax.dot_general(
            cols_ref[i], gall[i], (((0,), (0,)), ((), ())), preferred_element_type=f32
        )
        total = term if total is None else total + term
    wsend[...] = total.astype(bf16).reshape(sp, rows, 2 * latent)
    w_copies = send_all("sp", lambda p: wsend.at[p], lambda m: wall.at[m], sems, 4)
    wall[me_sp] = wsend[me_sp]
    for i in range(dp):
        hsend[i] = lax.dot_general(
            gall[i], w_ref[...], (((1,), (1,)), ((), ())), preferred_element_type=f32
        ).astype(bf16)
    h_copies = send_all(
        "dp", lambda p: hsend.at[p], lambda m: dh_ref.at[:, lanes_of(m, cw)], sems, 5
    )
    dh_ref[:, lanes_of(me_dp, cw)] = hsend[me_dp]
    received(w_copies)
    share = wall[0].astype(f32)
    for j in range(1, sp):
        share = share + wall[j].astype(f32)
    ssend[...] = share.astype(bf16)
    s_copies = send_all("sp", lambda p: ssend, lambda m: tall.at[m], sems, 6)
    tall[me_sp] = ssend[...]
    received(s_copies)
    for j in range(sp):
        dwb_ref[j] = tall[j, :, :latent].astype(f32)
        dwc_ref[j] = tall[j, :, latent:].astype(f32)
    for copies in (dx_copies, ddt_copies, h_copies):
        received(copies)
    for copies in (
        dbc_copies,
        dx_copies,
        ddt_copies,
        g_copies,
        w_copies,
        h_copies,
        s_copies,
    ):
        for copy in copies:
            copy.wait_send()


def comm_call(kernel, args, shapes, scratch, slots, peers, number, name):
    vmem = pl.BlockSpec(memory_space=pltpu.VMEM)
    return pl.pallas_call(
        kernel,
        in_specs=[vmem] * len(args),
        out_specs=[vmem] * len(shapes),
        out_shape=[jax.ShapeDtypeStruct(shape, kind) for shape, kind in shapes],
        scratch_shapes=[pltpu.VMEM(shape, bf16) for shape in scratch]
        + [pltpu.SemaphoreType.DMA((slots, 2, peers))],
        compiler_params=pltpu.CompilerParams(
            collective_id=number, has_side_effects=True, vmem_limit_bytes=60 * 1024 * 1024
        ),
        name=name,
    )(*args)


def local(
    layer_activity,
    writer_matrix,
    reader_matrix,
    source_unfiltered,
    switch_raw_signal,
    saved_result,
    final_adjoint,
    delta_raw,
    extra_logdrop,
    source_filter_coefs,
    writer_filter_coefs,
    reader_filter_coefs,
    delta_offset,
    fading_exponents,
    direct_factor,
    rescale_factor,
):
    tokens = layer_activity.shape[1]
    width_in = layer_activity.shape[2]
    latent = GROUPS * STATE
    dp = lax.axis_size("dp")
    sp = lax.axis_size("sp")
    heads = delta_offset.shape[0]
    per_group = HEADS // GROUPS
    xc = heads * HEAD_DIM
    xw = -(-xc // LANES) * LANES
    window = tokens * sp
    cw = width_in // dp
    peers = max(sp, dp)

    weights = jnp.concatenate([writer_matrix, reader_matrix], axis=1)
    x_by = pad_last(by_owner(source_unfiltered.reshape(tokens, INNER), sp), xw)
    dt_by = delta_raw.reshape(tokens, HEADS).T.reshape(sp, heads, tokens)
    dt_by = jnp.pad(dt_by, ((0, 0), (0, DT_ROWS - heads), (0, 0)))
    cols, x_all, dt_all, dy_all, bc_all, d_gate = comm_call(
        functools.partial(front_kernel, heads),
        (
            layer_activity.reshape(tokens, width_in),
            weights,
            x_by,
            dt_by,
            saved_result.reshape(tokens, INNER),
            switch_raw_signal.reshape(tokens, INNER),
            final_adjoint.reshape(tokens, INNER),
            rescale_factor.reshape(1, INNER),
        ),
        (
            ((dp, tokens, cw), bf16),
            ((sp, tokens, xw), bf16),
            ((sp, DT_ROWS, tokens), bf16),
            ((sp, tokens, xw), bf16),
            ((sp, tokens, 2 * STATE), bf16),
            ((tokens, INNER), bf16),
        ),
        (
            (sp, tokens, xw),
            (dp, tokens, 2 * latent),
            (dp, tokens, 2 * latent),
            (GROUPS, tokens, 2 * STATE),
        ),
        6,
        peers,
        0,
        "front",
    )

    group = lax.axis_index("sp") * heads // per_group
    tapbc = jnp.concatenate(
        [
            lax.dynamic_slice_in_dim(writer_filter_coefs, group * STATE, STATE, axis=1),
            lax.dynamic_slice_in_dim(reader_filter_coefs, group * STATE, STATE, axis=1),
        ],
        axis=1,
    )
    par = pad_last(jnp.stack([delta_offset, jnp.exp(fading_exponents)]), LANES)
    dx, dbc, ddt = mixer_backward(
        x_all.reshape(window, xw),
        dt_all,
        dy_all.reshape(window, xw),
        bc_all.reshape(window, 2 * STATE),
        pad_last(extra_logdrop.reshape(window, heads), LANES),
        pad_last(
            jnp.concatenate([source_filter_coefs, jnp.repeat(direct_factor, HEAD_DIM)[None]]), xw
        ),
        tapbc,
        par,
        heads,
    )
    rows = cw // sp
    back_x, back_dt, d_hidden, d_w_b, d_w_c = comm_call(
        functools.partial(back_kernel, heads),
        (
            dx.reshape(sp, tokens, xw),
            dbc.reshape(sp, tokens, 2 * STATE),
            ddt,
            cols,
            weights,
        ),
        (
            ((tokens, INNER) if xc % LANES == 0 else (sp, tokens, xw), bf16),
            ((sp, DT_ROWS, tokens), bf16),
            ((tokens, width_in), bf16),
            ((sp, rows, latent), f32),
            ((sp, rows, latent), f32),
        ),
        (
            (sp, tokens, 2 * STATE),
            (dp, tokens, 2 * latent),
            (tokens, 2 * latent),
            (sp, rows, 2 * latent),
            (sp, rows, 2 * latent),
            (dp, tokens, cw),
            (rows, 2 * latent),
            (sp, rows, 2 * latent),
        ),
        7,
        peers,
        1,
        "back",
    )
    if xc % LANES:
        back_x = jnp.transpose(back_x[:, :, :xc], (1, 0, 2))
    back_dt = back_dt[:, :heads].reshape(HEADS, tokens).T
    return (
        d_hidden.reshape(1, tokens, width_in),
        back_x.reshape(1, tokens, INNER),
        d_gate.reshape(1, tokens, INNER),
        back_dt.reshape(1, tokens, HEADS),
        d_w_b.reshape(cw, latent),
        d_w_c.reshape(cw, latent),
    )


def solution(mesh):
    in_specs = (
        P("dp", "sp", None),
        P("dp", None),
        P("dp", None),
        P("dp", "sp", None),
        P("dp", "sp", None),
        P("dp", "sp", None),
        P("dp", "sp", None),
        P("dp", "sp", None),
        P("dp", None, "sp"),
        P(None, "sp"),
        P(),
        P(),
        P("sp"),
        P("sp"),
        P("sp"),
        P(),
    )
    out_specs = (
        P("dp", "sp", None),
        P("dp", "sp", None),
        P("dp", "sp", None),
        P("dp", "sp", None),
        P("dp", None),
        P("dp", None),
    )
    return jax.shard_map(local, mesh=mesh, in_specs=in_specs, out_specs=out_specs, check_vma=False)
```
